32 devices in a mesh: gr: 2 (over x), fs: 8 (over z, y), tp: 2 (over core).
Axes of the slice: x: 2, y: 2, z: 4, core: 2. Of those that a mesh axis runs over, the one named last changes fastest.
Arguments:
- tokens: bfloat16 [4096, 2048], P(('gr', 'tp'), 'fs'), may hold values from -400 to 400
- norm_gain: float32 [2048], P('fs'), may hold values from 0.1 to 1.9
- up_weight: float32 [2048, 8192], P('fs', ('gr', 'tp')), may hold values from -0.125 to 0.125
- down_weight: float32 [8192, 2048], P('fs', ('gr', 'tp')), may hold values from -0.09375 to 0.09375
Outputs:
- mixed: bfloat16 [2048, 4096], P('fs', ('gr', 'tp'))
- up_ready: bfloat16 [2048, 8192], P(None, 'fs')
- down_ready: bfloat16 [8192, 2048], P('fs')
The draws below stay inside these ranges and needn't reach their ends.
All inputs are finite; a program needn't handle non-finite values.
Results may differ from the reference program's by a relative error of at most 0.023.
Values may be sent and summed in bfloat16 or wider, within the bound.
A program may use at most 64 MiB of HBM per device.

```python
import math
import jax
import jax.numpy as jnp
from jax import lax

D = 2048
FF = 8192
TOKENS = 4096
N_FS = 8


def draw_tokens(key, part):
    keys = jax.random.split(key, 3)
    row_scales = jnp.exp(jax.random.uniform(keys[0], (TOKENS, 1), jnp.float32) * math.log(10.0))
    column_scales = jnp.exp(jax.random.uniform(keys[1], (1, D), jnp.float32) * math.log(10.0))
    base = jax.random.truncated_normal(keys[2], -4.0, 4.0, (TOKENS, D), jnp.float32)
    return (base * row_scales * column_scales).astype(jnp.bfloat16)


def with_spikes(array, key, source, target, shards_of, factor):
    def block_of(axis_at):
        return (jnp.arange(array.shape[axis_at]) // (array.shape[axis_at] // shards_of)).reshape((-1,) + (1,) * (array.ndim - 1 - axis_at))

    one_side = jax.random.permutation(key, shards_of)[block_of(target)]
    other_side = (block_of(target) + shards_of // 2) % shards_of
    return jnp.where((block_of(source) == one_side) | (block_of(source) == other_side), factor * array, array)


def steps_of(own_key, shape, shards, least, largest):
    def one(position, parts):
        draws = jax.random.uniform(jax.random.fold_in(jax.random.fold_in(own_key, 6), position), (parts,), jnp.float32, least / len(shards), largest / len(shards))
        return jnp.repeat(jnp.exp(draws), shape[position] // parts).reshape((-1,) + (1,) * (len(shape) - position - 1))

    factor_of = one(*shards[0])
    for cut in shards[1:]:
        factor_of = factor_of * one(*cut)
    return factor_of


def scatter_about(stream_key, shape, scale, most, pieces=(), kind=jnp.bfloat16):
    drawn = jax.random.normal(stream_key, shape, jnp.float32) * scale
    if len(pieces) > 0:
        drawn = steps_of(stream_key, shape, pieces, -0.22, 0.18) * drawn
    return jnp.clip(drawn, min=-most, max=most).astype(kind)


def gaussian_with(own_key, shape, scale, bound, cuts, heavy, kind=jnp.bfloat16):
    entries = scale * jax.random.normal(own_key, shape, jnp.float32)
    if cuts:
        entries = entries * steps_of(own_key, shape, cuts, -0.22, 0.18)
    return jnp.clip(with_spikes(entries, jax.random.fold_in(own_key, 3), *heavy), -bound, bound).astype(kind)


def setup_inputs(seed: int = 0) -> dict:
    arg_keys = jax.random.split(jax.random.key(seed), 5)
    return {
        "tokens": draw_tokens(jax.random.fold_in(arg_keys[4], 71), 0),
        "norm_gain": jnp.clip(1.0 + 0.18 * jax.random.normal(arg_keys[1], (D,), jnp.float32), 0.1, 1.9),
        "up_weight": scatter_about(arg_keys[2], (D, FF), D ** -0.5, 0.125, ((0, 8), (1, 4)), jnp.float32),
        "down_weight": gaussian_with(arg_keys[3], (FF, D), FF ** -0.5, 0.09375, ((0, 8), (1, 4)), (0, 1, 8, 2.0), jnp.float32),
    }


epsilon = 1e-06

def reference(tokens, norm_gain, up_weight, down_weight):
    up_ready = (norm_gain[:, None] * up_weight).astype(jnp.bfloat16)
    down_ready = down_weight.astype(jnp.bfloat16)
    raw_up = jnp.dot(tokens, up_ready, preferred_element_type=jnp.float32)
    widened = tokens.astype(jnp.float32)
    row_scale = lax.rsqrt(lax.optimization_barrier(jnp.mean(widened * widened, axis=1)) + epsilon)
    hidden = jnp.square(jax.nn.relu(raw_up * row_scale[:, None])).astype(jnp.bfloat16)
    block = FF // N_FS

    def add_block(running, index):
        start = (index * block).astype(jnp.int32)
        piece = lax.dynamic_slice_in_dim(hidden, start, block, 1)
        weight_rows = lax.dynamic_slice_in_dim(down_ready, start, block, 0)
        partial_value = jnp.dot(piece, weight_rows, preferred_element_type=jnp.float32).astype(jnp.bfloat16)
        partial_value = lax.optimization_barrier(partial_value).astype(jnp.float32)
        return (running + partial_value, None)
    running, _ = lax.scan(add_block, jnp.zeros((TOKENS, D), jnp.float32), jnp.arange(N_FS, dtype=jnp.int32))
    return (running.T.astype(jnp.bfloat16), up_ready, down_ready)
```

```python
import functools

import jax
import jax.numpy as jnp
from jax import lax
from jax.experimental import pallas as pl
from jax.experimental.pallas import tpu as pltpu
from jax.sharding import PartitionSpec as P

MESH = pl.DeviceIdType.MESH
epsilon = 1e-06


def line_shape(count):
    short = max(d for d in range(1, count + 1) if count % d == 0 and d * d <= count)
    return count // short, short


def chunks(total, size):
    return min(total, size)


def kernel(
    G, n, T, Z, Y, k,
    tok_ref, gain_ref, upw_ref, dnw_ref,
    mixed_ref, up_out, dn_out,
    up_bf, tok_full, up_full, dn_full, hidden, part, ybuf, zup, zdn,
    tok_recv, tok_su, tok_sd, tok_sy,
    up_recv, up_s, up_sx, up_st,
    dn_recv, dn_sx, dn_st,
    y_recv, y_send, zu_recv, zu_send, zd_recv, zd_send, out_sem,
):
    g, f, t = lax.axis_index("gr"), lax.axis_index("fs"), lax.axis_index("tp")
    z, y = f // Y, f % Y
    q = g * T + t
    rows = upw_ref.shape[0]
    sub = rows // G
    unit = up_full.shape[1]
    dcols = dnw_ref.shape[1]
    pending = []

    def send(src, dst, ssem, rsem, dev, cond=None):
        copy = pltpu.make_async_remote_copy(
            src_ref=src, dst_ref=dst, send_sem=ssem, recv_sem=rsem, device_id=dev, device_id_type=MESH
        )
        if cond is None:
            copy.start()
        else:
            pl.when(cond)(copy.start)
        pending.append((cond, copy))

    def arrived(ref, sem):
        pltpu.make_async_copy(ref, ref, sem).wait()

    own = pltpu.make_async_copy(tok_ref, tok_full.at[f], tok_recv.at[f])
    own.start()

    def pass_tokens(zc, src, up, down):
        c = zc * Y + y
        dst = tok_full.at[c]
        if up is not None:
            send(src, dst, tok_su.at[zc], tok_recv.at[c], (g, f + Y, t), up)
        if down is not None:
            send(src, dst, tok_sd.at[zc], tok_recv.at[c], (g, f - Y, t), down)

    def cross_tokens(zc, src, cond):
        c = zc * Y + y
        for o in range(1, Y):
            y2 = (y + o) % Y
            send(src, tok_full.at[c], tok_sy.at[zc, o], tok_recv.at[c], (g, z * Y + y2, t), cond)

    pass_tokens(z, tok_ref, z < Z - 1, z > 0)
    cross_tokens(z, tok_ref, None)

    step = chunks(rows, 32)
    for j in range(k):
        @pl.loop(0, rows // step)
        def _(i):
            r = pl.ds(pl.multiple_of(i * step, step), step)
            up_bf[j, r, :] = (gain_ref[r, :] * upw_ref[r, pl.ds(j * unit, unit)]).astype(jnp.bfloat16)

    def piece(c, h):
        return up_full.at[pl.ds(pl.multiple_of(c * rows + h * sub, sub), sub)]

    for oh in reversed(range(G)):
        h = (g + oh) % G
        for j in range(k):
            owner = q * k + j
            src = up_bf.at[j, pl.ds(pl.multiple_of(h * sub, sub), sub)]
            if oh == 0:
                local = pltpu.make_async_copy(src, piece(f, h), up_recv.at[f, h])
                pl.when(owner == f)(local.start)
                send(src, piece(f, h), up_s.at[j, oh], up_recv.at[f, h], (h, owner, t), owner != f)
            else:
                send(src, piece(f, h), up_s.at[j, oh], up_recv.at[f, h], (h, owner, t))

    def dn_block(index):
        return dn_full.at[:, pl.ds(pl.multiple_of(index * dcols, dcols), dcols)]

    deep = dnw_ref.shape[0]
    dstep = chunks(deep, 64)

    @pl.loop(0, deep // dstep)
    def _(i):
        r = pl.ds(pl.multiple_of(i * dstep, dstep), dstep)
        dn_full[r, pl.ds(pl.multiple_of(q * dcols, dcols), dcols)] = dnw_ref[r, :].astype(jnp.bfloat16)

    for o in range(1, G):
        send(dn_block(q), dn_block(q), dn_sx.at[o], dn_recv.at[q], ((g + o) % G, f, t))
    for o in range(1, T):
        send(dn_block(q), dn_block(q), dn_st.at[0, o], dn_recv.at[q], (g, f, (t + o) % T))

    star = (f // k) % T
    is_star = t == star

    def relay_direct(c):
        @pl.when(is_star)
        def _():
            arrived(piece(c, g), up_recv.at[c, g])
        for o in range(1, G):
            send(piece(c, g), piece(c, g), up_sx.at[c, o], up_recv.at[c, g], ((g + o) % G, f, t), is_star)
        for o in range(1, T):
            send(piece(c, g), piece(c, g), up_st.at[c, 0, o], up_recv.at[c, g], (g, f, (t + o) % T), is_star)

    def relay_far(c):
        for oh in range(1, G):
            h = (g + oh) % G
            @pl.when(is_star)
            def _():
                arrived(piece(c, h), up_recv.at[c, h])
            for o in range(1, T):
                send(piece(c, h), piece(c, h), up_st.at[c, oh, o], up_recv.at[c, h], (g, f, (t + o) % T), is_star)

    earlier = []
    for s in range(Z):
        if s > 0:
            lower, upper = z - s >= 0, z + s < Z
            zl, zu = jnp.maximum(z - s, 0), jnp.minimum(z + s, Z - 1)

            @pl.when(lower)
            def _():
                arrived(tok_full.at[zl * Y + y], tok_recv.at[zl * Y + y])
            pass_tokens(zl, tok_full.at[zl * Y + y], lower & (z < Z - 1), None)
            cross_tokens(zl, tok_full.at[zl * Y + y], lower)

            @pl.when(upper)
            def _():
                arrived(tok_full.at[zu * Y + y], tok_recv.at[zu * Y + y])
            pass_tokens(zu, tok_full.at[zu * Y + y], None, upper & (z > 0))
            cross_tokens(zu, tok_full.at[zu * Y + y], upper)
        else:
            own.wait()
        zc = (z + s) % Z
        now = [zc * Y + (y + o) % Y for o in range(Y)]
        for c in now:
            relay_direct(c)
        for c in earlier:
            relay_far(c)
        earlier = now
        if s == 1 % Z:
            for o in range(1, G):
                index = ((g + o) % G) * T + t
                arrived(dn_block(index), dn_recv.at[index])
                for ot in range(1, T):
                    send(dn_block(index), dn_block(index), dn_st.at[o, ot], dn_recv.at[index], (g, f, (t + ot) % T))
    for c in earlier:
        relay_far(c)

    for zc in range(Z):
        for o in range(1, Y):
            c = zc * Y + (y + o) % Y
            arrived(tok_full.at[c], tok_recv.at[c])

    @pl.when(jnp.logical_not(is_star))
    def _():
        @pl.loop(0, n)
        def _(c):
            for h in range(G):
                arrived(piece(c, h), up_recv.at[c, h])

    up_store = pltpu.make_async_copy(up_full, up_out, out_sem.at[0])
    up_store.start()

    tokens_here = tok_ref.shape[0]
    tile = chunks(tokens_here, 256)
    width = n * tok_ref.shape[1]

    @pl.loop(0, tokens_here // tile)
    def _(i):
        r = pl.ds(pl.multiple_of(i * tile, tile), tile)
        blocks = [tok_full[c, r, :] for c in range(n)]
        squares = None
        for block in blocks:
            wide = block.astype(jnp.float32)
            total = jnp.sum(wide * wide, axis=1, keepdims=True)
            squares = total if squares is None else squares + total
        scale = lax.rsqrt(squares / width + epsilon)
        raw = jnp.dot(jnp.concatenate(blocks, axis=1), up_full[...], preferred_element_type=jnp.float32)
        hidden[r, :] = jnp.square(jnp.maximum(raw * scale, 0.0)).astype(jnp.bfloat16)

    for o in range(G):
        for ot in range(1, T):
            index = ((g + o) % G) * T + (t + ot) % T
            arrived(dn_block(index), dn_recv.at[index])
    dn_store = pltpu.make_async_copy(dn_full, dn_out, out_sem.at[1])
    dn_store.start()

    feat = part.shape[1]

    def nth(o):
        value = jnp.int32(0)
        for zv in range(Z):
            order = sorted(range(Z), key=lambda zd: (-abs(zd - zv), zd))
            value = jnp.where(z == zv, order[o], value)
        return value

    def multiply(c):
        across = dn_full[:, pl.ds(pl.multiple_of(c * feat, feat), feat)] if feat % 128 == 0 else None
        return across

    if feat % 128 == 0:
        def compute(c):
            cols = dn_full[:, pl.ds(pl.multiple_of(c * feat, feat), feat)]
            part[c] = lax.dot_general(
                cols.T, hidden[...], (((1,), (1,)), ((), ())), preferred_element_type=jnp.float32
            ).astype(jnp.bfloat16)
    else:
        per = 128 // feat

        @pl.loop(0, n // per)
        def _(b):
            cols = dn_full[:, pl.ds(pl.multiple_of(b * 128, 128), 128)]
            whole = lax.dot_general(
                cols.T, hidden[...], (((1,), (1,)), ((), ())), preferred_element_type=jnp.float32
            ).astype(jnp.bfloat16)
            for p in range(per):
                part[b * per + p] = whole[p * feat:(p + 1) * feat]

        def compute(c):
            pass

    @pl.loop(0, Z)
    def _(i):
        zd = nth_dynamic(i, z, Z)
        for o in range(1, Y):
            y2 = (y + o) % Y
            c = zd * Y + y2
            compute(c)
            pltpu.make_async_remote_copy(
                src_ref=part.at[c], dst_ref=ybuf.at[zd, Y - o], send_sem=y_send.at[zd, o],
                recv_sem=y_recv.at[zd, Y - o], device_id=(g, z * Y + y2, t), device_id_type=MESH,
            ).start()
        compute(zd * Y + y)

    for zd in range(Z):
        for o in range(1, Y):
            c = zd * Y + (y + o) % Y
            pending.append((None, pltpu.make_async_remote_copy(
                src_ref=part.at[c], dst_ref=ybuf.at[zd, Y - o], send_sem=y_send.at[zd, o],
                recv_sem=y_recv.at[zd, Y - o], device_id=(g, z * Y + (y + o) % Y, t), device_id_type=MESH,
            )))

    rstep = chunks(feat, 32)

    def add_up(zd, extras, target, start=None):
        c = zd * Y + y

        @pl.loop(0, feat // rstep)
        def _(i):
            r = pl.ds(pl.multiple_of(i * rstep, rstep), rstep)
            total = part[c, r, :].astype(jnp.float32)
            for o in range(1, Y):
                total = total + ybuf[zd, o, r, :].astype(jnp.float32)
            for extra in extras:
                total = total + extra[zd, r, :].astype(jnp.float32)
            if target is None:
                part[c, r, :] = total.astype(jnp.bfloat16)
            else:
                target[r, :] = total.astype(jnp.bfloat16)

    for i in range(Z):
        zd = nth(i)
        for o in range(1, Y):
            arrived(ybuf.at[zd, o], y_recv.at[zd, o])
        c = zd * Y + y
        going_up, going_down = zd > z, zd < z

        @pl.when(going_up & (z > 0))
        def _():
            arrived(zup.at[zd], zu_recv.at[zd])
            add_up(zd, [zup], None)

        @pl.when(going_up & (z == 0))
        def _():
            add_up(zd, [], None)

        @pl.when(going_down & (z < Z - 1))
        def _():
            arrived(zdn.at[zd], zd_recv.at[zd])
            add_up(zd, [zdn], None)

        @pl.when(going_down & (z == Z - 1))
        def _():
            add_up(zd, [], None)

        send(part.at[c], zup.at[zd], zu_send.at[zd], zu_recv.at[zd], (g, f + Y, t), going_up)
        send(part.at[c], zdn.at[zd], zd_send.at[zd], zd_recv.at[zd], (g, f - Y, t), going_down)

        @pl.when(zd == z)
        def _():
            @pl.when(z > 0)
            def _():
                arrived(zup.at[zd], zu_recv.at[zd])

            @pl.when(z < Z - 1)
            def _():
                arrived(zdn.at[zd], zd_recv.at[zd])

            @pl.when(z == 0)
            def _():
                add_up(zd, [zdn] if Z > 1 else [], mixed_ref)

            if Z > 1:
                @pl.when(z == Z - 1)
                def _():
                    add_up(zd, [zup], mixed_ref)

                @pl.when((z > 0) & (z < Z - 1))
                def _():
                    add_up(zd, [zup, zdn], mixed_ref)

    for cond, copy in pending:
        if cond is None:
            copy.wait_send()
        else:
            pl.when(cond)(copy.wait_send)
    up_store.wait()
    dn_store.wait()


def nth_dynamic(i, z, Z):
    value = jnp.int32(0)
    for zv in range(Z):
        order = sorted(range(Z), key=lambda zd: (-abs(zd - zv), zd))
        for o in range(Z):
            value = jnp.where((z == zv) & (i == o), order[o], value)
    return value


def shards(dims, tokens, norm_gain, up_weight, down_weight):
    G, n, T = dims
    Z, Y = line_shape(n)
    rows, cols = up_weight.shape
    here, w = tokens.shape
    deep, dcols = down_weight.shape
    unit = cols * G * T // n
    k = n // (G * T)
    width = rows * n
    feat = dcols * G * T // n
    bf = jnp.bfloat16
    dma = pltpu.SemaphoreType.DMA
    vmem = pl.BlockSpec(memory_space=pltpu.VMEM)
    hbm = pl.BlockSpec(memory_space=pl.ANY)
    return pl.pallas_call(
        functools.partial(kernel, G, n, T, Z, Y, k),
        out_shape=(
            jax.ShapeDtypeStruct((feat, here), bf),
            jax.ShapeDtypeStruct((width, unit), bf),
            jax.ShapeDtypeStruct((deep, dcols * G * T), bf),
        ),
        in_specs=[vmem] * 4,
        out_specs=(vmem, hbm, hbm),
        scratch_shapes=[
            pltpu.VMEM((k, rows, unit), bf),
            pltpu.VMEM((n, here, w), bf),
            pltpu.VMEM((width, unit), bf),
            pltpu.VMEM((deep, dcols * G * T), bf),
            pltpu.VMEM((here, unit), bf),
            pltpu.VMEM((n, feat, here), bf),
            pltpu.VMEM((Z, Y, feat, here), bf),
            pltpu.VMEM((Z, feat, here), bf),
            pltpu.VMEM((Z, feat, here), bf),
            dma((n,)), dma((Z,)), dma((Z,)), dma((Z, Y)),
            dma((n, G)), dma((k, G)), dma((n, G)), dma((n, G, T)),
            dma((G * T,)), dma((G,)), dma((G, T)),
            dma((Z, Y)), dma((Z, Y)), dma((Z,)), dma((Z,)), dma((Z,)), dma((Z,)), dma((2,)),
        ],
        compiler_params=pltpu.CompilerParams(has_side_effects=True, vmem_limit_bytes=60 * 1024 * 1024),
    )(tokens, norm_gain[:, None], up_weight, down_weight)


def solution(mesh):
    dims = (mesh.shape["gr"], mesh.shape["fs"], mesh.shape["tp"])
    in_specs = (P(("gr", "tp"), "fs"), P("fs"), P("fs", ("gr", "tp")), P("fs", ("gr", "tp")))
    out_specs = (P("fs", ("gr", "tp")), P(None, "fs"), P("fs", None))
    return jax.shard_map(
        functools.partial(shards, dims), mesh=mesh, in_specs=in_specs, out_specs=out_specs, check_vma=False
    )
```

```python
import functools

import jax
import jax.numpy as jnp
from jax import lax
from jax.experimental import pallas as pl
from jax.experimental.pallas import tpu as pltpu
from jax.sharding import PartitionSpec as P

MESH = pl.DeviceIdType.MESH
epsilon = 1e-06


def line_shape(count):
    short = max(d for d in range(1, count + 1) if count % d == 0 and d * d <= count)
    return count // short, short


def chunks(total, size):
    return min(total, size)


def kernel(
    G, n, T, Z, Y, k,
    tok_ref, gain_ref, upw_ref, dnw_ref,
    mixed_ref, up_full, dn_full,
    up_bf, xbuf, tok_full, hidden, part, ybuf, zup, zdn,
    tok_recv, tok_su, tok_sd, tok_sy,
    x_recv, x_send, up_recv, up_s, up_sx, up_st,
    dn_recv, dn_sx, dn_st,
    y_recv, y_send, zu_recv, zu_send, zd_recv, zd_send,
):
    g, f, t = lax.axis_index("gr"), lax.axis_index("fs"), lax.axis_index("tp")
    z, y = f // Y, f % Y
    q = g * T + t
    rows = upw_ref.shape[0]
    sub = rows // G
    unit = up_full.shape[1]
    dcols = dnw_ref.shape[1]
    pending = []

    def send(src, dst, ssem, rsem, dev, cond=None):
        copy = pltpu.make_async_remote_copy(
            src_ref=src, dst_ref=dst, send_sem=ssem, recv_sem=rsem, device_id=dev, device_id_type=MESH
        )
        if cond is None:
            copy.start()
        else:
            pl.when(cond)(copy.start)
        pending.append((cond, copy))

    def arrived(ref, sem):
        pltpu.make_async_copy(ref, ref, sem).wait()

    own = pltpu.make_async_copy(tok_ref, tok_full.at[f], tok_recv.at[f])
    own.start()

    def pass_tokens(zc, src, up, down):
        c = zc * Y + y
        dst = tok_full.at[c]
        if up is not None:
            send(src, dst, tok_su.at[zc], tok_recv.at[c], (g, f + Y, t), up)
        if down is not None:
            send(src, dst, tok_sd.at[zc], tok_recv.at[c], (g, f - Y, t), down)

    def cross_tokens(zc, src, cond):
        c = zc * Y + y
        for o in range(1, Y):
            y2 = (y + o) % Y
            send(src, tok_full.at[c], tok_sy.at[zc, o], tok_recv.at[c], (g, z * Y + y2, t), cond)

    pass_tokens(z, tok_ref, z < Z - 1, z > 0)
    cross_tokens(z, tok_ref, None)

    step = chunks(rows, 32)
    for j in range(k):
        @pl.loop(0, rows // step)
        def _(i):
            r = pl.ds(pl.multiple_of(i * step, step), step)
            up_bf[j, r, :] = (gain_ref[r, :] * upw_ref[r, pl.ds(j * unit, unit)]).astype(jnp.bfloat16)

    def piece(c, h):
        return up_full.at[pl.ds(pl.multiple_of(c * rows + h * sub, sub), sub)]

    def to_owner(j, slot, source_q, src):
        owner = source_q * k + j
        local = pltpu.make_async_copy(src, piece(f, g), up_recv.at[f, g])
        pl.when(owner == f)(local.start)
        send(src, piece(f, g), up_s.at[j, slot], up_recv.at[f, g], (g, owner, t), owner != f)

    def half(j, h):
        return up_bf.at[j, pl.ds(pl.multiple_of(h * sub, sub), sub)]

    for oh in range(1, G):
        h = (g + oh) % G
        for j in range(k):
            send(half(j, h), xbuf.at[G - oh, j], x_send.at[j, oh], x_recv.at[j, G - oh], (h, f, t))
    for j in range(k):
        to_owner(j, 0, q, half(j, g))

    def dn_block(index):
        return dn_full.at[:, pl.ds(pl.multiple_of(index * dcols, dcols), dcols)]

    deep = dnw_ref.shape[0]
    dstep = chunks(deep, 64)

    @pl.loop(0, deep // dstep)
    def _(i):
        r = pl.ds(pl.multiple_of(i * dstep, dstep), dstep)
        dn_full[r, pl.ds(pl.multiple_of(q * dcols, dcols), dcols)] = dnw_ref[r, :].astype(jnp.bfloat16)

    for o in range(1, G):
        send(dn_block(q), dn_block(q), dn_sx.at[o], dn_recv.at[q], ((g + o) % G, f, t))
    for o in range(1, T):
        send(dn_block(q), dn_block(q), dn_st.at[0, o], dn_recv.at[q], (g, f, (t + o) % T))

    star = (f // k) % T
    is_star = t == star

    def relay_direct(c, cond):
        ok = is_star & cond

        @pl.when(ok)
        def _():
            arrived(piece(c, g), up_recv.at[c, g])
        for o in range(1, G):
            send(piece(c, g), piece(c, g), up_sx.at[c, o], up_recv.at[c, g], ((g + o) % G, f, t), ok)
        for o in range(1, T):
            send(piece(c, g), piece(c, g), up_st.at[c, 0, o], up_recv.at[c, g], (g, f, (t + o) % T), ok)

    def relay_far(c, cond):
        ok = is_star & cond
        for oh in range(1, G):
            h = (g + oh) % G

            @pl.when(ok)
            def _():
                arrived(piece(c, h), up_recv.at[c, h])
            for o in range(1, T):
                send(piece(c, h), piece(c, h), up_st.at[c, oh, o], up_recv.at[c, h], (g, f, (t + o) % T), ok)

    for og in range(1, G):
        for j in range(k):
            arrived(xbuf.at[og, j], x_recv.at[j, og])
            to_owner(j, og, ((g + og) % G) * T + t, xbuf.at[og, j])
    own.wait()

    earlier = []
    for s in range(Z):
        now = []
        if s == 0:
            now = [(z * Y + (y + o) % Y, True) for o in range(Y)]
        else:
            lower, upper = z - s >= 0, z + s < Z
            zl, zu = jnp.maximum(z - s, 0), jnp.minimum(z + s, Z - 1)

            @pl.when(lower)
            def _():
                arrived(tok_full.at[zl * Y + y], tok_recv.at[zl * Y + y])
            pass_tokens(zl, tok_full.at[zl * Y + y], lower & (z < Z - 1), None)
            cross_tokens(zl, tok_full.at[zl * Y + y], lower)

            @pl.when(upper)
            def _():
                arrived(tok_full.at[zu * Y + y], tok_recv.at[zu * Y + y])
            pass_tokens(zu, tok_full.at[zu * Y + y], None, upper & (z > 0))
            cross_tokens(zu, tok_full.at[zu * Y + y], upper)
            for o in range(Y):
                now.append((zl * Y + (y + o) % Y, lower))
                now.append((zu * Y + (y + o) % Y, upper))
        for c, cond in now:
            relay_direct(c, cond)
        for c, cond in earlier:
            relay_far(c, cond)
        earlier = now
        if s == 1 % Z:
            for o in range(1, G):
                index = ((g + o) % G) * T + t
                arrived(dn_block(index), dn_recv.at[index])
                for ot in range(1, T):
                    send(dn_block(index), dn_block(index), dn_st.at[o, ot], dn_recv.at[index], (g, f, (t + ot) % T))
    for c, cond in earlier:
        relay_far(c, cond)

    for zc in range(Z):
        for o in range(1, Y):
            c = zc * Y + (y + o) % Y
            arrived(tok_full.at[c], tok_recv.at[c])

    @pl.when(jnp.logical_not(is_star))
    def _():
        @pl.loop(0, n)
        def _(c):
            for h in range(G):
                arrived(piece(c, h), up_recv.at[c, h])

    tokens_here = tok_ref.shape[0]
    tile = chunks(tokens_here, 256)
    width = n * tok_ref.shape[1]

    @pl.loop(0, tokens_here // tile)
    def _(i):
        r = pl.ds(pl.multiple_of(i * tile, tile), tile)
        blocks = [tok_full[c, r, :] for c in range(n)]
        squares = None
        for block in blocks:
            wide = block.astype(jnp.float32)
            total = jnp.sum(wide * wide, axis=1, keepdims=True)
            squares = total if squares is None else squares + total
        scale = lax.rsqrt(squares / width + epsilon)
        raw = jnp.dot(jnp.concatenate(blocks, axis=1), up_full[...], preferred_element_type=jnp.float32)
        hidden[r, :] = jnp.square(jnp.maximum(raw * scale, 0.0)).astype(jnp.bfloat16)

    for o in range(G):
        for ot in range(1, T):
            index = ((g + o) % G) * T + (t + ot) % T
            arrived(dn_block(index), dn_recv.at[index])

    feat = part.shape[1]

    def nth(o):
        value = jnp.int32(0)
        for zv in range(Z):
            order = sorted(range(Z), key=lambda zd: (-abs(zd - zv), zd))
            value = jnp.where(z == zv, order[o], value)
        return value

    if feat % 128 == 0:
        def compute(c):
            cols = dn_full[:, pl.ds(pl.multiple_of(c * feat, feat), feat)]
            part[c] = lax.dot_general(
                cols.T, hidden[...], (((1,), (1,)), ((), ())), preferred_element_type=jnp.float32
            ).astype(jnp.bfloat16)
    else:
        per = 128 // feat

        @pl.loop(0, n // per)
        def _(b):
            cols = dn_full[:, pl.ds(pl.multiple_of(b * 128, 128), 128)]
            whole = lax.dot_general(
                cols.T, hidden[...], (((1,), (1,)), ((), ())), preferred_element_type=jnp.float32
            ).astype(jnp.bfloat16)
            for p in range(per):
                part[b * per + p] = whole[p * feat:(p + 1) * feat]

        def compute(c):
            pass

    @pl.loop(0, Z)
    def _(i):
        zd = nth_dynamic(i, z, Z)
        for o in range(1, Y):
            y2 = (y + o) % Y
            c = zd * Y + y2
            compute(c)
            pltpu.make_async_remote_copy(
                src_ref=part.at[c], dst_ref=ybuf.at[zd, Y - o], send_sem=y_send.at[zd, o],
                recv_sem=y_recv.at[zd, Y - o], device_id=(g, z * Y + y2, t), device_id_type=MESH,
            ).start()
        compute(zd * Y + y)

    for zd in range(Z):
        for o in range(1, Y):
            c = zd * Y + (y + o) % Y
            pending.append((None, pltpu.make_async_remote_copy(
                src_ref=part.at[c], dst_ref=ybuf.at[zd, Y - o], send_sem=y_send.at[zd, o],
                recv_sem=y_recv.at[zd, Y - o], device_id=(g, z * Y + (y + o) % Y, t), device_id_type=MESH,
            )))

    rstep = chunks(feat, 32)

    def add_up(zd, extras, target, start=None):
        c = zd * Y + y

        @pl.loop(0, feat // rstep)
        def _(i):
            r = pl.ds(pl.multiple_of(i * rstep, rstep), rstep)
            total = part[c, r, :].astype(jnp.float32)
            for o in range(1, Y):
                total = total + ybuf[zd, o, r, :].astype(jnp.float32)
            for extra in extras:
                total = total + extra[zd, r, :].astype(jnp.float32)
            if target is None:
                part[c, r, :] = total.astype(jnp.bfloat16)
            else:
                target[r, :] = total.astype(jnp.bfloat16)

    for i in range(Z):
        zd = nth(i)
        for o in range(1, Y):
            arrived(ybuf.at[zd, o], y_recv.at[zd, o])
        c = zd * Y + y
        going_up, going_down = zd > z, zd < z

        @pl.when(going_up & (z > 0))
        def _():
            arrived(zup.at[zd], zu_recv.at[zd])
            add_up(zd, [zup], None)

        @pl.when(going_up & (z == 0))
        def _():
            add_up(zd, [], None)

        @pl.when(going_down & (z < Z - 1))
        def _():
            arrived(zdn.at[zd], zd_recv.at[zd])
            add_up(zd, [zdn], None)

        @pl.when(going_down & (z == Z - 1))
        def _():
            add_up(zd, [], None)

        send(part.at[c], zup.at[zd], zu_send.at[zd], zu_recv.at[zd], (g, f + Y, t), going_up)
        send(part.at[c], zdn.at[zd], zd_send.at[zd], zd_recv.at[zd], (g, f - Y, t), going_down)

        @pl.when(zd == z)
        def _():
            @pl.when(z > 0)
            def _():
                arrived(zup.at[zd], zu_recv.at[zd])

            @pl.when(z < Z - 1)
            def _():
                arrived(zdn.at[zd], zd_recv.at[zd])

            @pl.when(z == 0)
            def _():
                add_up(zd, [zdn] if Z > 1 else [], mixed_ref)

            if Z > 1:
                @pl.when(z == Z - 1)
                def _():
                    add_up(zd, [zup], mixed_ref)

                @pl.when((z > 0) & (z < Z - 1))
                def _():
                    add_up(zd, [zup, zdn], mixed_ref)

    for cond, copy in pending:
        if cond is None:
            copy.wait_send()
        else:
            pl.when(cond)(copy.wait_send)


def nth_dynamic(i, z, Z):
    value = jnp.int32(0)
    for zv in range(Z):
        order = sorted(range(Z), key=lambda zd: (-abs(zd - zv), zd))
        for o in range(Z):
            value = jnp.where((z == zv) & (i == o), order[o], value)
    return value


def shards(dims, tokens, norm_gain, up_weight, down_weight):
    G, n, T = dims
    Z, Y = line_shape(n)
    rows, cols = up_weight.shape
    here, w = tokens.shape
    deep, dcols = down_weight.shape
    unit = cols * G * T // n
    k = n // (G * T)
    width = rows * n
    feat = dcols * G * T // n
    bf = jnp.bfloat16
    dma = pltpu.SemaphoreType.DMA
    vmem = pl.BlockSpec(memory_space=pltpu.VMEM)
    hbm = pl.BlockSpec(memory_space=pl.ANY)
    return pl.pallas_call(
        functools.partial(kernel, G, n, T, Z, Y, k),
        out_shape=(
            pltpu.VMEM((feat, here), bf),
            pltpu.VMEM((width, unit), bf),
            pltpu.VMEM((deep, dcols * G * T), bf),
        ),
        in_specs=[vmem] * 4,
        out_specs=(vmem, vmem, vmem),
        scratch_shapes=[
            pltpu.VMEM((k, rows, unit), bf),
            pltpu.VMEM((G, k, rows // G, unit), bf),
            pltpu.VMEM((n, here, w), bf),
            pltpu.VMEM((here, unit), bf),
            pltpu.VMEM((n, feat, here), bf),
            pltpu.VMEM((Z, Y, feat, here), bf),
            pltpu.VMEM((Z, feat, here), bf),
            pltpu.VMEM((Z, feat, here), bf),
            dma((n,)), dma((Z,)), dma((Z,)), dma((Z, Y)),
            dma((k, G)), dma((k, G)), dma((n, G)), dma((k, G)), dma((n, G)), dma((n, G, T)),
            dma((G * T,)), dma((G,)), dma((G, T)),
            dma((Z, Y)), dma((Z, Y)), dma((Z,)), dma((Z,)), dma((Z,)), dma((Z,)),
        ],
        compiler_params=pltpu.CompilerParams(has_side_effects=True, vmem_limit_bytes=46 * 1024 * 1024),
    )(tokens, norm_gain[:, None], up_weight, down_weight)


def solution(mesh):
    dims = (mesh.shape["gr"], mesh.shape["fs"], mesh.shape["tp"])
    in_specs = (P(("gr", "tp"), "fs"), P("fs"), P("fs", ("gr", "tp")), P("fs", ("gr", "tp")))
    out_specs = (P("fs", ("gr", "tp")), P(None, "fs"), P("fs", None))
    return jax.shard_map(
        functools.partial(shards, dims), mesh=mesh, in_specs=in_specs, out_specs=out_specs, check_vma=False
    )
```

```python
import functools

import jax
import jax.numpy as jnp
from jax import lax
from jax.experimental import pallas as pl
from jax.experimental.pallas import tpu as pltpu
from jax.sharding import PartitionSpec as P

MESH = pl.DeviceIdType.MESH
epsilon = 1e-06


def line_shape(count):
    short = max(d for d in range(1, count + 1) if count % d == 0 and d * d <= count)
    return count // short, short


def chunks(total, size):
    return min(total, size)


def kernel(
    G, n, T, Z, Y, k, E,
    tok_ref, gain_ref, upw_ref, dnw_ref,
    mixed_ref, up_full, dn_full,
    up_bf, xbuf, tok_full, hidden, part, ybuf, zup, zdn,
    tok_recv, tok_su, tok_sd, tok_sy,
    x_recv, x_send, up_recv, up_s, up_sx, up_st,
    dn_recv, dn_sx, dn_st,
    y_recv, y_send, zu_recv, zu_send, zd_recv, zd_send,
):
    g, f, t = lax.axis_index("gr"), lax.axis_index("fs"), lax.axis_index("tp")
    z, y = f // Y, f % Y
    q = g * T + t
    rows = upw_ref.shape[0]
    sub = rows // G
    unit = up_full.shape[1]
    dcols = dnw_ref.shape[1]
    pending = []

    def send(src, dst, ssem, rsem, dev, cond=None):
        copy = pltpu.make_async_remote_copy(
            src_ref=src, dst_ref=dst, send_sem=ssem, recv_sem=rsem, device_id=dev, device_id_type=MESH
        )
        if cond is None:
            copy.start()
        else:
            pl.when(cond)(copy.start)
        pending.append((cond, copy))

    def arrived(ref, sem):
        pltpu.make_async_copy(ref, ref, sem).wait()

    slab = tok_ref.shape[0] // E

    def owns(e):
        return pltpu.make_async_copy(tok_ref.at[pl.ds(e * slab, slab)], tok(f, e), tok_recv.at[f, e])

    def tok(c, e):
        return tok_full.at[c, pl.ds(e * slab, slab)]

    for e in range(E):
        owns(e).start()

    def pass_tokens(zc, e, src, up, down):
        c = zc * Y + y
        dst = tok(c, e)
        if up is not None:
            send(src, dst, tok_su.at[zc, e], tok_recv.at[c, e], (g, f + Y, t), up)
        if down is not None:
            send(src, dst, tok_sd.at[zc, e], tok_recv.at[c, e], (g, f - Y, t), down)

    def cross_tokens(zc, e, src, cond):
        c = zc * Y + y
        for o in range(1, Y):
            y2 = (y + o) % Y
            send(src, tok(c, e), tok_sy.at[zc, o, e], tok_recv.at[c, e], (g, z * Y + y2, t), cond)

    for e in range(E):
        mine = tok_ref.at[pl.ds(e * slab, slab)]
        pass_tokens(z, e, mine, z < Z - 1, z > 0)
        cross_tokens(z, e, mine, None)

    step = chunks(rows, 32)
    for j in range(k):
        @pl.loop(0, rows // step)
        def _(i):
            r = pl.ds(pl.multiple_of(i * step, step), step)
            up_bf[j, r, :] = (gain_ref[r, :] * upw_ref[r, pl.ds(j * unit, unit)]).astype(jnp.bfloat16)

    def piece(c, h):
        return up_full.at[pl.ds(pl.multiple_of(c * rows + h * sub, sub), sub)]

    def to_owner(j, slot, source_q, src):
        owner = source_q * k + j
        local = pltpu.make_async_copy(src, piece(f, g), up_recv.at[f, g])
        pl.when(owner == f)(local.start)
        send(src, piece(f, g), up_s.at[j, slot], up_recv.at[f, g], (g, owner, t), owner != f)

    def half(j, h):
        return up_bf.at[j, pl.ds(pl.multiple_of(h * sub, sub), sub)]

    for oh in range(1, G):
        h = (g + oh) % G
        for j in range(k):
            send(half(j, h), xbuf.at[G - oh, j], x_send.at[j, oh], x_recv.at[j, G - oh], (h, f, t))
    for j in range(k):
        to_owner(j, 0, q, half(j, g))

    def dn_block(index):
        return dn_full.at[:, pl.ds(pl.multiple_of(index * dcols, dcols), dcols)]

    deep = dnw_ref.shape[0]
    dstep = chunks(deep, 64)

    @pl.loop(0, deep // dstep)
    def _(i):
        r = pl.ds(pl.multiple_of(i * dstep, dstep), dstep)
        dn_full[r, pl.ds(pl.multiple_of(q * dcols, dcols), dcols)] = dnw_ref[r, :].astype(jnp.bfloat16)

    for o in range(1, G):
        send(dn_block(q), dn_block(q), dn_sx.at[o], dn_recv.at[q], ((g + o) % G, f, t))
    for o in range(1, T):
        send(dn_block(q), dn_block(q), dn_st.at[0, o], dn_recv.at[q], (g, f, (t + o) % T))

    star = (f // k) % T
    is_star = t == star

    def relay_direct(c, cond):
        ok = is_star & cond

        @pl.when(ok)
        def _():
            arrived(piece(c, g), up_recv.at[c, g])
        for o in range(1, G):
            send(piece(c, g), piece(c, g), up_sx.at[c, o], up_recv.at[c, g], ((g + o) % G, f, t), ok)
        for o in range(1, T):
            send(piece(c, g), piece(c, g), up_st.at[c, 0, o], up_recv.at[c, g], (g, f, (t + o) % T), ok)

    def relay_far(c, cond):
        ok = is_star & cond
        for oh in range(1, G):
            h = (g + oh) % G

            @pl.when(ok)
            def _():
                arrived(piece(c, h), up_recv.at[c, h])
            for o in range(1, T):
                send(piece(c, h), piece(c, h), up_st.at[c, oh, o], up_recv.at[c, h], (g, f, (t + o) % T), ok)

    for og in range(1, G):
        for j in range(k):
            arrived(xbuf.at[og, j], x_recv.at[j, og])
            to_owner(j, og, ((g + og) % G) * T + t, xbuf.at[og, j])
    for e in range(E):
        owns(e).wait()

    earlier = []
    for s in range(Z):
        now = []
        if s == 0:
            now = [(z * Y + (y + o) % Y, True) for o in range(Y)]
        else:
            lower, upper = z - s >= 0, z + s < Z
            zl, zu = jnp.maximum(z - s, 0), jnp.minimum(z + s, Z - 1)

            for e in range(E):
                @pl.when(lower)
                def _():
                    arrived(tok(zl * Y + y, e), tok_recv.at[zl * Y + y, e])
                pass_tokens(zl, e, tok(zl * Y + y, e), lower & (z < Z - 1), None)
                cross_tokens(zl, e, tok(zl * Y + y, e), lower)

                @pl.when(upper)
                def _():
                    arrived(tok(zu * Y + y, e), tok_recv.at[zu * Y + y, e])
                pass_tokens(zu, e, tok(zu * Y + y, e), None, upper & (z > 0))
                cross_tokens(zu, e, tok(zu * Y + y, e), upper)
            for o in range(Y):
                now.append((zl * Y + (y + o) % Y, lower))
                now.append((zu * Y + (y + o) % Y, upper))
        for c, cond in now:
            relay_direct(c, cond)
        for c, cond in earlier:
            relay_far(c, cond)
        earlier = now
        if s == 1 % Z:
            for o in range(1, G):
                index = ((g + o) % G) * T + t
                arrived(dn_block(index), dn_recv.at[index])
                for ot in range(1, T):
                    send(dn_block(index), dn_block(index), dn_st.at[o, ot], dn_recv.at[index], (g, f, (t + ot) % T))
    for c, cond in earlier:
        relay_far(c, cond)

    for zc in range(Z):
        for o in range(1, Y):
            c = zc * Y + (y + o) % Y
            for e in range(E):
                arrived(tok(c, e), tok_recv.at[c, e])

    @pl.when(jnp.logical_not(is_star))
    def _():
        @pl.loop(0, n)
        def _(c):
            for h in range(G):
                arrived(piece(c, h), up_recv.at[c, h])

    tokens_here = tok_ref.shape[0]
    tile = chunks(tokens_here, 256)
    width = n * tok_ref.shape[1]

    @pl.loop(0, tokens_here // tile)
    def _(i):
        r = pl.ds(pl.multiple_of(i * tile, tile), tile)
        blocks = [tok_full[c, r, :] for c in range(n)]
        squares = None
        for block in blocks:
            wide = block.astype(jnp.float32)
            total = jnp.sum(wide * wide, axis=1, keepdims=True)
            squares = total if squares is None else squares + total
        scale = lax.rsqrt(squares / width + epsilon)
        raw = jnp.dot(jnp.concatenate(blocks, axis=1), up_full[...], preferred_element_type=jnp.float32)
        hidden[r, :] = jnp.square(jnp.maximum(raw * scale, 0.0)).astype(jnp.bfloat16)

    for o in range(G):
        for ot in range(1, T):
            index = ((g + o) % G) * T + (t + ot) % T
            arrived(dn_block(index), dn_recv.at[index])

    feat = part.shape[1]

    def nth(o):
        value = jnp.int32(0)
        for zv in range(Z):
            order = sorted(range(Z), key=lambda zd: (-abs(zd - zv), zd))
            value = jnp.where(z == zv, order[o], value)
        return value

    if feat % 128 == 0:
        def compute(c):
            cols = dn_full[:, pl.ds(pl.multiple_of(c * feat, feat), feat)]
            part[c] = lax.dot_general(
                cols.T, hidden[...], (((1,), (1,)), ((), ())), preferred_element_type=jnp.float32
            ).astype(jnp.bfloat16)
    else:
        per = 128 // feat

        @pl.loop(0, n // per)
        def _(b):
            cols = dn_full[:, pl.ds(pl.multiple_of(b * 128, 128), 128)]
            whole = lax.dot_general(
                cols.T, hidden[...], (((1,), (1,)), ((), ())), preferred_element_type=jnp.float32
            ).astype(jnp.bfloat16)
            for p in range(per):
                part[b * per + p] = whole[p * feat:(p + 1) * feat]

        def compute(c):
            pass

    @pl.loop(0, Z)
    def _(i):
        zd = nth_dynamic(i, z, Z)
        for o in range(1, Y):
            y2 = (y + o) % Y
            c = zd * Y + y2
            compute(c)
            pltpu.make_async_remote_copy(
                src_ref=part.at[c], dst_ref=ybuf.at[zd, Y - o], send_sem=y_send.at[zd, o],
                recv_sem=y_recv.at[zd, Y - o], device_id=(g, z * Y + y2, t), device_id_type=MESH,
            ).start()
        compute(zd * Y + y)

    for zd in range(Z):
        for o in range(1, Y):
            c = zd * Y + (y + o) % Y
            pending.append((None, pltpu.make_async_remote_copy(
                src_ref=part.at[c], dst_ref=ybuf.at[zd, Y - o], send_sem=y_send.at[zd, o],
                recv_sem=y_recv.at[zd, Y - o], device_id=(g, z * Y + (y + o) % Y, t), device_id_type=MESH,
            )))

    rstep = chunks(feat, 32)

    def add_up(zd, extras, target, start=None):
        c = zd * Y + y

        @pl.loop(0, feat // rstep)
        def _(i):
            r = pl.ds(pl.multiple_of(i * rstep, rstep), rstep)
            total = part[c, r, :].astype(jnp.float32)
            for o in range(1, Y):
                total = total + ybuf[zd, o, r, :].astype(jnp.float32)
            for extra in extras:
                total = total + extra[zd, r, :].astype(jnp.float32)
            if target is None:
                part[c, r, :] = total.astype(jnp.bfloat16)
            else:
                target[r, :] = total.astype(jnp.bfloat16)

    for i in range(Z):
        zd = nth(i)
        for o in range(1, Y):
            arrived(ybuf.at[zd, o], y_recv.at[zd, o])
        c = zd * Y + y
        going_up, going_down = zd > z, zd < z

        @pl.when(going_up & (z > 0))
        def _():
            arrived(zup.at[zd], zu_recv.at[zd])
            add_up(zd, [zup], None)

        @pl.when(going_up & (z == 0))
        def _():
            add_up(zd, [], None)

        @pl.when(going_down & (z < Z - 1))
        def _():
            arrived(zdn.at[zd], zd_recv.at[zd])
            add_up(zd, [zdn], None)

        @pl.when(going_down & (z == Z - 1))
        def _():
            add_up(zd, [], None)

        send(part.at[c], zup.at[zd], zu_send.at[zd], zu_recv.at[zd], (g, f + Y, t), going_up)
        send(part.at[c], zdn.at[zd], zd_send.at[zd], zd_recv.at[zd], (g, f - Y, t), going_down)

        @pl.when(zd == z)
        def _():
            @pl.when(z > 0)
            def _():
                arrived(zup.at[zd], zu_recv.at[zd])

            @pl.when(z < Z - 1)
            def _():
                arrived(zdn.at[zd], zd_recv.at[zd])

            @pl.when(z == 0)
            def _():
                add_up(zd, [zdn] if Z > 1 else [], mixed_ref)

            if Z > 1:
                @pl.when(z == Z - 1)
                def _():
                    add_up(zd, [zup], mixed_ref)

                @pl.when((z > 0) & (z < Z - 1))
                def _():
                    add_up(zd, [zup, zdn], mixed_ref)

    for cond, copy in pending:
        if cond is None:
            copy.wait_send()
        else:
            pl.when(cond)(copy.wait_send)


def nth_dynamic(i, z, Z):
    value = jnp.int32(0)
    for zv in range(Z):
        order = sorted(range(Z), key=lambda zd: (-abs(zd - zv), zd))
        for o in range(Z):
            value = jnp.where((z == zv) & (i == o), order[o], value)
    return value


def shards(dims, tokens, norm_gain, up_weight, down_weight):
    G, n, T = dims
    Z, Y = line_shape(n)
    rows, cols = up_weight.shape
    here, w = tokens.shape
    deep, dcols = down_weight.shape
    unit = cols * G * T // n
    k = n // (G * T)
    E = 2 if here % 64 == 0 else 1
    width = rows * n
    feat = dcols * G * T // n
    bf = jnp.bfloat16
    dma = pltpu.SemaphoreType.DMA
    vmem = pl.BlockSpec(memory_space=pltpu.VMEM)
    hbm = pl.BlockSpec(memory_space=pl.ANY)
    return pl.pallas_call(
        functools.partial(kernel, G, n, T, Z, Y, k, E),
        out_shape=(
            pltpu.VMEM((feat, here), bf),
            pltpu.VMEM((width, unit), bf),
            pltpu.VMEM((deep, dcols * G * T), bf),
        ),
        in_specs=[vmem] * 4,
        out_specs=(vmem, vmem, vmem),
        scratch_shapes=[
            pltpu.VMEM((k, rows, unit), bf),
            pltpu.VMEM((G, k, rows // G, unit), bf),
            pltpu.VMEM((n, here, w), bf),
            pltpu.VMEM((here, unit), bf),
            pltpu.VMEM((n, feat, here), bf),
            pltpu.VMEM((Z, Y, feat, here), bf),
            pltpu.VMEM((Z, feat, here), bf),
            pltpu.VMEM((Z, feat, here), bf),
            dma((n, E)), dma((Z, E)), dma((Z, E)), dma((Z, Y, E)),
            dma((k, G)), dma((k, G)), dma((n, G)), dma((k, G)), dma((n, G)), dma((n, G, T)),
            dma((G * T,)), dma((G,)), dma((G, T)),
            dma((Z, Y)), dma((Z, Y)), dma((Z,)), dma((Z,)), dma((Z,)), dma((Z,)),
        ],
        compiler_params=pltpu.CompilerParams(has_side_effects=True, vmem_limit_bytes=46 * 1024 * 1024),
    )(tokens, norm_gain[:, None], up_weight, down_weight)


def solution(mesh):
    dims = (mesh.shape["gr"], mesh.shape["fs"], mesh.shape["tp"])
    in_specs = (P(("gr", "tp"), "fs"), P("fs"), P("fs", ("gr", "tp")), P("fs", ("gr", "tp")))
    out_specs = (P("fs", ("gr", "tp")), P(None, "fs"), P("fs", None))
    return jax.shard_map(
        functools.partial(shards, dims), mesh=mesh, in_specs=in_specs, out_specs=out_specs, check_vma=False
    )
```
